32 devices in a mesh: ep: 8 (over z, x), tp: 4 (over y, core).
Axes of the slice: x: 2, y: 2, z: 4, core: 2. Of those that a mesh axis runs over, the one named last changes fastest.
Arguments:
- hidden_in: bfloat16 [256, 4096], P('ep'), may hold values from -6 to 6
- norm_gain: float32 [4096], replicated, may hold values from 0.1 to 1.9
- group_ids: int32 [256], P('ep'), may hold values from 0 to 1, as said below
- inner_ids: int32 [256, 4], P('ep'), may hold values from 0 to 7, as said below
- group_prob: float32 [256], P('ep'), may hold values from 0.25 to 1
- expert_prob: float32 [256, 4], P('ep'), may hold values from 0.1 to 1
- w_gate: bfloat16 [16, 4096, 1024], P('ep', None, 'tp'), may hold values from -0.09375 to 0.09375
- w_up: bfloat16 [16, 4096, 1024], P('ep', None, 'tp'), may hold values from -0.09375 to 0.09375
- w_down: bfloat16 [16, 1024, 4096], P('ep', None, 'tp'), may hold values from -0.1875 to 0.1875
Outputs:
- moe_out: bfloat16 [256, 4096], P('ep', 'tp')
The draws below stay inside these ranges and needn't reach their ends.
Inputs may be any that keep to these rules, and one draw needn't show every extreme that they name: `group_ids`: among the 32 tokens of one index of ep no group is named by more than 16 tokens; one group is named by exactly 16 of them, and all of these name one common expert of it. `inner_ids`: each row names 4 different experts of the token's group.
All inputs are finite; a program needn't handle non-finite values.
Results may differ from the reference program's by a relative error of at most 0.0069.
Values may be sent and summed in bfloat16 or wider, within the bound.
A program may use at most 64 MiB of HBM per device.

```python
import jax
import jax.numpy as jnp
from jax import lax

D = 4096
DE = 1024
EPG = 8
TOP = 4
TOK_DEV = 32
CAP = 16
EXPERTS = 16
GROUPS = 2
TOKENS = 256


def routing(key):
    subkeys = jax.random.split(jax.random.fold_in(key, 7), 8)
    block_count = TOKENS // TOK_DEV
    group_order = jax.random.permutation(subkeys[0], GROUPS)
    chosen = jnp.minimum(jax.random.randint(subkeys[1], (block_count,), 0, GROUPS), jax.random.randint(subkeys[2], (block_count,), 0, GROUPS))
    hot_group = group_order[chosen]
    others = jax.random.randint(subkeys[3], (block_count, TOK_DEV), 0, GROUPS - 1)
    others = jnp.where(others >= hot_group[:, None], others + 1, others)
    places = jax.vmap(lambda single: jax.random.permutation(single, TOK_DEV))(jax.random.split(subkeys[4], block_count))
    forced = places < CAP
    groups = jnp.where(forced, hot_group[:, None], others)
    inner = jax.vmap(lambda single: jax.random.permutation(single, EPG))(jax.random.split(subkeys[5], TOKENS))[:, :TOP]
    inner = inner.reshape(block_count, TOK_DEV, TOP)
    common = jax.random.randint(subkeys[6], (block_count,), 0, EPG)
    contains = jnp.any(inner == common[:, None, None], axis=-1)
    first = jnp.where(forced & jnp.logical_not(contains), common[:, None], inner[:, :, 0])
    inner = inner.at[:, :, 0].set(first)
    return (groups.reshape(TOKENS).astype(jnp.int32), inner.reshape(TOKENS, TOP).astype(jnp.int32))


def draw_group_ids(key, part):
    return routing(key)[0]


def draw_inner_ids(key, part):
    return routing(key)[1]


def block_scale(rng, extent, pieces, smallest, largest):
    level = 1.0
    for dim, shards_of in pieces:
        draws = jax.random.uniform(jax.random.fold_in(jax.random.fold_in(rng, 6), dim), (shards_of,), jnp.float32, smallest / len(pieces), largest / len(pieces))
        level = level * jnp.repeat(jnp.exp(draws), extent[dim] // shards_of).reshape((-1,) + (1,) * (len(extent) - 1 - dim))
    return level


def gaussian(key, extent, width, reach, cuts=(), kind=jnp.bfloat16):
    entries = width * jax.random.normal(key, extent, jnp.float32)
    if cuts:
        entries = entries * block_scale(key, extent, cuts, -0.22, 0.18)
    return jnp.clip(entries, -reach, reach).astype(kind)


def setup_inputs(seed: int = 0) -> dict:
    keys = jax.random.split(jax.random.key(seed), 10)
    hidden_in = gaussian(keys[0], (TOKENS, D), 1.0, 6.0, ((0, 8),))
    norm_gain = jnp.clip(1.0 + 0.18 * jax.random.normal(keys[1], (D,), jnp.float32), 0.1, 1.9)
    group_ids = draw_group_ids(jax.random.fold_in(keys[9], 71), 0)
    inner_ids = draw_inner_ids(jax.random.fold_in(keys[9], 71), 0)
    group_prob = jnp.clip(0.25 + 0.75 * jax.random.uniform(keys[4], (TOKENS,), jnp.float32) ** block_scale(keys[4], (TOKENS,), ((0, 8),), -0.2, 0.2), 0.25, 1.0)
    expert_prob = jnp.clip(0.1 + 0.9 * jax.random.uniform(keys[5], (TOKENS, TOP), jnp.float32) ** block_scale(keys[5], (TOKENS, TOP), ((0, 8),), -0.2, 0.2), 0.1, 1.0)
    w_gate = gaussian(keys[6], (EXPERTS, D, DE), D ** -0.5, 0.09375, ((0, 8), (2, 4)))
    w_up = gaussian(keys[7], (EXPERTS, D, DE), D ** -0.5, 0.09375, ((0, 8), (2, 4)))
    w_down = gaussian(keys[8], (EXPERTS, DE, D), DE ** -0.5, 0.1875, ((0, 8), (2, 4)))
    return {"hidden_in": hidden_in, "norm_gain": norm_gain, "group_ids": group_ids, "inner_ids": inner_ids, "group_prob": group_prob, "expert_prob": expert_prob, "w_gate": w_gate, "w_up": w_up, "w_down": w_down}


EPS = 1e-06

def reference(hidden_in, norm_gain, group_ids, inner_ids, group_prob, expert_prob, w_gate, w_up, w_down):
    widened = hidden_in.astype(jnp.float32)
    normed = (widened * lax.rsqrt(lax.optimization_barrier(jnp.mean(widened * widened, axis=-1, keepdims=True)) + EPS) * norm_gain).astype(jnp.bfloat16)
    expert_ids = group_ids[:, None] * EPG + inner_ids
    scaled = group_prob[:, None] * expert_prob
    route = lax.optimization_barrier(jnp.sum(jax.nn.one_hot(expert_ids, EXPERTS, dtype=jnp.float32) * scaled[:, :, None], axis=1))

    def one_expert(combined, inputs):
        gate_w, up_w, down_w, column = inputs
        gate_proj = jnp.dot(normed, gate_w, preferred_element_type=jnp.float32)
        up_proj = jnp.dot(normed, up_w, preferred_element_type=jnp.float32)
        activation = (jax.nn.silu(gate_proj) * up_proj * column[:, None]).astype(jnp.bfloat16)
        return (combined + jnp.dot(activation, down_w, preferred_element_type=jnp.float32), None)
    start = jnp.zeros((TOKENS, D), jnp.float32)
    combined, _ = lax.scan(one_expert, start, (w_gate, w_up, w_down, route.T))
    return combined.astype(jnp.bfloat16)
```

```python
import functools

import jax
import jax.numpy as jnp
from jax import lax
from jax.experimental import pallas as pl
from jax.experimental.pallas import tpu as pltpu
from jax.sharding import PartitionSpec as P

EPG = 8
EPS = 1e-06
CORES = 2
LANES = 128
MESH = pl.DeviceIdType.MESH


def rem(value, count):
    return lax.rem(value + count, count)


def moe_kernel(
    ep_count, tp_count,
    hid_ref, gain_ref, grp_ref, inner_ref, gprob_ref, eprob_ref, wg_hbm, wu_hbm, wd_hbm,
    out_ref,
    wg, wu, wd, rows_out, rows_in, acts, parts, back,
    w_sem, a_send, a_recv, b_send, b_recv, r_send, r_recv,
    h_send, h_recv, hr_send, hr_recv, o_send, o_recv,
):
    experts, depth, hidden = wg.shape
    ranks = EPG // experts
    groups = ep_count // ranks
    ys = tp_count // CORES
    tokens = hid_ref.shape[0]
    cap = tokens // 2
    feats = depth // tp_count
    cols = wd.shape[2]

    me_ep, me_tp = lax.axis_index("ep"), lax.axis_index("tp")
    g, p = lax.div(me_ep, ranks), lax.rem(me_ep, ranks)
    y, c = lax.div(me_tp, CORES), lax.rem(me_tp, CORES)
    sib = 1 - c

    loads = []
    for k, (src, dst) in enumerate(((wg_hbm, wg), (wu_hbm, wu), (wd_hbm, wd))):
        load = pltpu.make_async_copy(src, dst, w_sem.at[k])
        load.start()
        loads.append(load)

    barrier = pltpu.get_barrier_semaphore()
    partners = 0

    def shift(rank, d, sign):
        return rem(lax.div(rank, 2) + sign * (d // 2), ranks // 2) * 2 + rem(
            lax.rem(rank, 2) + sign * (d % 2), 2
        )

    def to(d):
        return shift(p, d, 1)

    def of(d):
        return shift(p, d, -1)

    def mate(j, rank):
        flip = groups == 2 and ranks > 2 and j == 1
        return shift(rank, ranks // 2, 1) if flip else rank

    def greet(ep, tp):
        pl.semaphore_signal(
            barrier, inc=1, device_id={"ep": ep, "tp": tp}, device_id_type=MESH
        )

    for d in range(1, ep_count):
        greet(rem(me_ep + d, ep_count), me_tp)
        partners += 1
    for d in range(ranks):
        for dy in range(1, ys):
            greet(g * ranks + to(d), rem(y + dy, ys) * CORES + c)
            partners += 1
    greet(me_ep, y * CORES + sib)
    partners += 1

    x = hid_ref[...].astype(jnp.float32)
    scale = lax.rsqrt(jnp.mean(x * x, axis=-1, keepdims=True) + EPS)
    mine = pl.ds(pl.multiple_of(me_tp * feats, LANES), feats)
    normed = (
        hid_ref[:, mine].astype(jnp.float32) * scale * gain_ref[:, mine]
    ).astype(jnp.bfloat16)

    r0 = lax.broadcasted_iota(jnp.int32, (tokens, tokens), 0)
    r1 = lax.broadcasted_iota(jnp.int32, (tokens, tokens), 1)
    grow = jnp.broadcast_to(grp_ref[...], (tokens, tokens))
    gcol = jnp.sum(jnp.where(r0 == r1, grow, 0), axis=1, keepdims=True)
    same = gcol == grow
    rank_row = jnp.sum(jnp.where(same & (r0 < r1), 1, 0), axis=0, keepdims=True)
    rank_col = jnp.sum(jnp.where(same & (r1 < r0), 1, 0), axis=1, keepdims=True)

    def slot(group, rank):
        rel = g - group
        return jnp.where(rel < 0, rel + groups, rel) * cap + rank

    slots = groups * cap
    pick = (
        lax.broadcasted_iota(jnp.int32, (slots, tokens), 0) == slot(grp_ref[...], rank_row)
    ).astype(jnp.bfloat16)

    line = lax.broadcasted_iota(jnp.int32, (LANES, tokens), 0)
    inner, eprob, prob = inner_ref[...], eprob_ref[...], gprob_ref[...]
    weight = jnp.zeros((LANES, tokens), jnp.float32)
    for k in range(inner.shape[0]):
        hit = lax.rem(line, EPG) == inner[k : k + 1, :]
        weight += jnp.where(hit, prob * eprob[k : k + 1, :], 0.0)
    high = weight.astype(jnp.bfloat16).astype(jnp.float32)
    mid = (weight - high).astype(jnp.bfloat16).astype(jnp.float32)
    low = weight - high - mid
    part = lax.div(line, EPG)
    weight = jnp.where(
        part == 0, high, jnp.where(part == 1, mid, jnp.where(part == 2, low, 0.0))
    ).astype(jnp.bfloat16)

    data = jnp.dot(pick, normed, preferred_element_type=jnp.float32).astype(jnp.bfloat16)
    wdat = lax.dot_general(
        pick, weight, (((1,), (1,)), ((), ())), preferred_element_type=jnp.float32
    ).astype(jnp.bfloat16)
    my_rows = pl.ds(pl.multiple_of(p * cap, cap), cap)
    rows_in[0, c, y, my_rows, :feats] = data[:cap]
    rows_in[0, c, y, my_rows, feats:] = wdat[:cap]
    for j in range(1, groups):
        rows_out[j, :, :feats] = data[j * cap : (j + 1) * cap]
        rows_out[j, :, feats:] = wdat[j * cap : (j + 1) * cap]

    pl.semaphore_wait(barrier, partners)
    sent = []

    def send(src, dst, ssem, rsem, ep, tp):
        copy = pltpu.make_async_remote_copy(
            src_ref=src, dst_ref=dst, send_sem=ssem, recv_sem=rsem,
            device_id={"ep": ep, "tp": tp}, device_id_type=MESH,
        )
        copy.start()
        sent.append(copy)

    def landed(dst, ssem, rsem):
        pltpu.make_async_remote_copy(
            src_ref=dst, dst_ref=dst, send_sem=ssem, recv_sem=rsem,
            device_id={"ep": me_ep, "tp": me_tp}, device_id_type=MESH,
        ).wait_recv()

    def piece(j, core, yy, rank):
        return rows_in.at[j, core, yy, pl.ds(pl.multiple_of(rank * cap, cap), cap)]

    hops = sorted(
        ((d, dy) for d in range(ranks) for dy in range(ys)),
        key=lambda h: (h != (0, 0), -(h[0] // 2 + h[0] % 2 + h[1])),
    )

    def spread(j):
        own = piece(j, c, y, p)
        for d, dy in hops[1:]:
            send(own, own, b_send.at[j, d, dy], b_recv.at[j, d, dy],
                 g * ranks + to(d), rem(y + dy, ys) * CORES + c)
        send(own, own, r_send.at[j, 0, 0], r_recv.at[j, 0, 0], me_ep, y * CORES + sib)

    def relay(j):
        for d, dy in hops[1:]:
            got = piece(j, c, rem(y - dy, ys), of(d))
            landed(got, b_send.at[j, d, dy], b_recv.at[j, d, dy])
            send(got, got, r_send.at[j, d, dy], r_recv.at[j, d, dy], me_ep, y * CORES + sib)

    def expand(j):
        gates = [jnp.zeros((ranks * cap, hidden), jnp.float32) for _ in range(experts)]
        ups = [jnp.zeros((ranks * cap, hidden), jnp.float32) for _ in range(experts)]
        for half in range(CORES):
            core = sib if half else c
            if half:
                for d, dy in hops:
                    landed(piece(j, sib, rem(y - dy, ys), of(d)),
                           r_send.at[j, d, dy], r_recv.at[j, d, dy])
            for yy in range(ys):
                lhs = rows_in[j, core, yy, :, :feats]
                ks = pl.ds(pl.multiple_of((yy * CORES + core) * feats, feats), feats)
                for e in range(experts):
                    gates[e] += jnp.dot(lhs, wg[e, ks, :], preferred_element_type=jnp.float32)
                    ups[e] += jnp.dot(lhs, wu[e, ks, :], preferred_element_type=jnp.float32)
        wrow = rows_in[j, 0, 0, :, feats:].astype(jnp.float32)
        lanes = lax.broadcasted_iota(jnp.int32, wrow.shape, 1)
        for e in range(experts):
            w = jnp.sum(
                jnp.where(lax.rem(lanes, EPG) == p * experts + e, wrow, 0.0),
                axis=1, keepdims=True,
            )
            act = gates[e] / (1.0 + jnp.exp(-gates[e])) * ups[e] * w
            acts[j, c, y, :, e * hidden : (e + 1) * hidden] = act.astype(jnp.bfloat16)
        own = acts.at[j, c, y]
        for dy in range(1, ys):
            send(own, own, h_send.at[j, dy], h_recv.at[j, dy], me_ep,
                 rem(y + dy, ys) * CORES + c)
        send(own, own, hr_send.at[j, 0], hr_recv.at[j, 0], me_ep, y * CORES + sib)

    def act_relay(j):
        for dy in range(1, ys):
            got = acts.at[j, c, rem(y - dy, ys)]
            landed(got, h_send.at[j, dy], h_recv.at[j, dy])
            send(got, got, hr_send.at[j, dy], hr_recv.at[j, dy], me_ep, y * CORES + sib)

    def contract(j):
        total = jnp.zeros((ranks * cap, cols), jnp.float32)
        for half in range(CORES):
            core = sib if half else c
            if half:
                for dy in range(ys):
                    landed(acts.at[j, sib, rem(y - dy, ys)], hr_send.at[j, dy], hr_recv.at[j, dy])
            for yy in range(ys):
                ks = pl.ds(pl.multiple_of((yy * CORES + core) * hidden, hidden), hidden)
                for e in range(experts):
                    total += jnp.dot(
                        acts[j, core, yy, :, e * hidden : (e + 1) * hidden],
                        wd[e, ks, :], preferred_element_type=jnp.float32,
                    )
        parts[j] = total.astype(jnp.bfloat16)
        source = rem(g + j, groups) * ranks
        for d in reversed(range(ranks)):
            rows = pl.ds(pl.multiple_of(to(d) * cap, cap), cap)
            if j == 0 and d == 0:
                back[0, p] = parts[0, rows, :]
            else:
                send(parts.at[j, rows], back.at[j, p], o_send.at[j, d], o_recv.at[j, d],
                     source + mate(j, to(d)), me_tp)

    for j in range(1, groups):
        send(rows_out.at[j], piece(j, c, y, mate(j, p)), a_send.at[j],
             a_recv.at[j], rem(g - j, groups) * ranks + mate(j, p), me_tp)
    spread(0)
    for j in range(groups):
        if j + 1 < groups:
            landed(piece(j + 1, c, y, p), a_send.at[j + 1], a_recv.at[j + 1])
            spread(j + 1)
        relay(j)
        if j == 0:
            loads[0].wait()
            loads[1].wait()
        expand(j)
        if j:
            act_relay(j - 1)
            if j == 1:
                loads[2].wait()
            contract(j - 1)
    act_relay(groups - 1)
    if groups == 1:
        loads[2].wait()
    contract(groups - 1)

    sums = []
    for j in range(groups):
        for d in range(ranks):
            if j or d:
                landed(back.at[j, shift(mate(j, p), d, -1)], o_send.at[j, d], o_recv.at[j, d])
        block = back[j, 0].astype(jnp.float32)
        for k in range(1, ranks):
            block += back[j, k].astype(jnp.float32)
        sums.append(block.astype(jnp.bfloat16))
    place = (
        lax.broadcasted_iota(jnp.int32, (tokens, slots), 1) == slot(gcol, rank_col)
    ).astype(jnp.bfloat16)
    out_ref[...] = jnp.dot(
        place, jnp.concatenate(sums, axis=0), preferred_element_type=jnp.float32
    ).astype(jnp.bfloat16)
    for copy in sent:
        copy.wait_send()


def solution(mesh):
    ep_count, tp_count = mesh.shape["ep"], mesh.shape["tp"]

    def on_device(
        hidden_in, norm_gain, group_ids, inner_ids, group_prob, expert_prob, w_gate, w_up, w_down
    ):
        tokens = hidden_in.shape[0]
        experts, depth, hidden = w_gate.shape
        cols = w_down.shape[2]
        ranks, cap = EPG // experts, tokens // 2
        groups, ys = ep_count // ranks, tp_count // CORES
        feats = depth // tp_count
        vmem = pl.BlockSpec(memory_space=pltpu.VMEM)
        hbm = pl.BlockSpec(memory_space=pl.ANY)
        dma = pltpu.SemaphoreType.DMA
        return pl.pallas_call(
            functools.partial(moe_kernel, ep_count, tp_count),
            out_shape=pltpu.VMEM((tokens, cols), jnp.bfloat16),
            in_specs=[vmem] * 6 + [hbm] * 3,
            out_specs=vmem,
            scratch_shapes=[
                pltpu.VMEM(w_gate.shape, jnp.bfloat16),
                pltpu.VMEM(w_up.shape, jnp.bfloat16),
                pltpu.VMEM(w_down.shape, jnp.bfloat16),
                pltpu.VMEM((groups, cap, feats + LANES), jnp.bfloat16),
                pltpu.VMEM((groups, CORES, ys, ranks * cap, feats + LANES), jnp.bfloat16),
                pltpu.VMEM((groups, CORES, ys, ranks * cap, experts * hidden), jnp.bfloat16),
                pltpu.VMEM((groups, ranks * cap, cols), jnp.bfloat16),
                pltpu.VMEM((groups, ranks, cap, cols), jnp.bfloat16),
                dma((3,)),
                dma((groups,)), dma((groups,)),
                dma((groups, ranks, ys)), dma((groups, ranks, ys)),
                dma((groups, ranks, ys)), dma((groups, ranks, ys)),
                dma((groups, ys)), dma((groups, ys)),
                dma((groups, ys)), dma((groups, ys)),
                dma((groups, ranks)), dma((groups, ranks)),
            ],
            compiler_params=pltpu.CompilerParams(
                collective_id=0, has_side_effects=True, vmem_limit_bytes=56 * 1024 * 1024
            ),
        )(
            hidden_in, norm_gain.reshape(1, depth), group_ids.reshape(1, tokens), inner_ids.T,
            group_prob.reshape(1, tokens), expert_prob.T, w_gate, w_up, w_down,
        )

    placed = (
        P("ep", None), P(), P("ep"), P("ep", None), P("ep"), P("ep", None),
        P("ep", None, "tp"), P("ep", None, "tp"), P("ep", None, "tp"),
    )
    return jax.shard_map(
        on_device, mesh=mesh, in_specs=placed, out_specs=P("ep", "tp"), check_vma=False
    )
```

```python
import functools

import jax
import jax.numpy as jnp
from jax import lax
from jax.experimental import pallas as pl
from jax.experimental.pallas import tpu as pltpu
from jax.sharding import PartitionSpec as P

EPG = 8
EPS = 1e-06
CORES = 2
LANES = 128
SPLIT = 1
MESH = pl.DeviceIdType.MESH


def rem(value, count):
    return lax.rem(value + count, count)


def moe_kernel(
    ep_count, tp_count,
    hid_hbm, gain_hbm, grp_hbm, inner_hbm, gprob_hbm, eprob_hbm, wg_hbm, wu_hbm, wd_hbm,
    out_ref,
    hid_ref, gain_ref, grp_ref, inner_ref, gprob_ref, eprob_ref,
    wg, wu, wd, rows_out, rows_own, rows_in, acts, parts, back,
    i_sem, w_sem, a_send, a_recv, s_send, s_recv, q_send, q_recv, b_send, b_recv, r_send, r_recv,
    h_send, h_recv, hr_send, hr_recv, o_send, o_recv,
):
    experts, depth, hidden = wg.shape
    ranks = EPG // experts
    groups = ep_count // ranks
    ys = tp_count // CORES
    tokens = hid_ref.shape[0]
    cap = tokens // 2
    feats = depth // tp_count
    side = depth // CORES
    cols = wd.shape[2]
    block = cols // SPLIT

    me_ep, me_tp = lax.axis_index("ep"), lax.axis_index("tp")
    g, p = lax.div(me_ep, ranks), lax.rem(me_ep, ranks)
    y, c = lax.div(me_tp, CORES), lax.rem(me_tp, CORES)
    sib = 1 - c

    barrier = pltpu.get_barrier_semaphore()
    partners = 0

    def shift(rank, d, sign):
        return rem(lax.div(rank, 2) + sign * (d // 2), ranks // 2) * 2 + rem(
            lax.rem(rank, 2) + sign * (d % 2), 2
        )

    def to(d):
        return shift(p, d, 1)

    def of(d):
        return shift(p, d, -1)

    def mate(j, rank):
        flip = groups == 2 and ranks > 2 and j == 1
        return shift(rank, ranks // 2, 1) if flip else rank

    def twin(dy=0):
        return rem(y + dy, ys) * CORES + sib

    def greet(ep, tp):
        pl.semaphore_signal(
            barrier, inc=1, device_id={"ep": ep, "tp": tp}, device_id_type=MESH
        )

    for d in range(1, ep_count):
        greet(rem(me_ep + d, ep_count), me_tp)
        partners += 1
    for j in range(1, groups):
        greet(rem(g - j, groups) * ranks + mate(j, p), twin())
        partners += 1
    for d in range(ranks):
        for dy in range(ys):
            greet(g * ranks + to(d), twin(dy))
            partners += 1

    fetched = []
    for k, (src, dst) in enumerate((
        (hid_hbm, hid_ref), (gain_hbm, gain_ref), (grp_hbm, grp_ref), (inner_hbm, inner_ref),
        (gprob_hbm, gprob_ref), (eprob_hbm, eprob_ref),
    )):
        load = pltpu.make_async_copy(src, dst, i_sem.at[k])
        load.start()
        fetched.append(load)
    for load in fetched:
        load.wait()
    loads = []
    for k, (src, dst) in enumerate(((wg_hbm, wg), (wu_hbm, wu), (wd_hbm, wd))):
        load = pltpu.make_async_copy(src, dst, w_sem.at[k])
        load.start()
        loads.append(load)

    r0 = lax.broadcasted_iota(jnp.int32, (tokens, tokens), 0)
    r1 = lax.broadcasted_iota(jnp.int32, (tokens, tokens), 1)
    grow = jnp.broadcast_to(grp_ref[...], (tokens, tokens))
    gcol = jnp.sum(jnp.where(r0 == r1, grow, 0), axis=1, keepdims=True)
    same = gcol == grow
    rank_row = jnp.sum(jnp.where(same & (r0 < r1), 1, 0), axis=0, keepdims=True)
    rank_col = jnp.sum(jnp.where(same & (r1 < r0), 1, 0), axis=1, keepdims=True)

    def slot(group, rank):
        rel = g - group
        return jnp.where(rel < 0, rel + groups, rel) * cap + rank

    slots = groups * cap
    pick = (
        lax.broadcasted_iota(jnp.int32, (slots, tokens), 0) == slot(grp_ref[...], rank_row)
    ).astype(jnp.bfloat16)

    line = lax.broadcasted_iota(jnp.int32, (LANES, tokens), 0)
    inner, eprob, prob = inner_ref[...], eprob_ref[...], gprob_ref[...]
    weight = jnp.zeros((LANES, tokens), jnp.float32)
    for k in range(inner.shape[0]):
        hit = lax.rem(line, EPG) == inner[k : k + 1, :]
        weight += jnp.where(hit, prob * eprob[k : k + 1, :], 0.0)
    high = weight.astype(jnp.bfloat16).astype(jnp.float32)
    mid = (weight - high).astype(jnp.bfloat16).astype(jnp.float32)
    low = weight - high - mid
    part = lax.div(line, EPG)
    weight = jnp.where(
        part == 0, high, jnp.where(part == 1, mid, jnp.where(part == 2, low, 0.0))
    ).astype(jnp.bfloat16)
    wdat = lax.dot_general(
        pick, weight, (((1,), (1,)), ((), ())), preferred_element_type=jnp.float32
    ).astype(jnp.bfloat16)

    x = hid_ref[...].astype(jnp.float32)
    scale = lax.rsqrt(jnp.mean(x * x, axis=-1, keepdims=True) + EPS)

    def normed(cut):
        return (
            hid_ref[:, cut].astype(jnp.float32) * scale * gain_ref[:, cut]
        ).astype(jnp.bfloat16)

    if groups > 1:
        mine = pl.ds(pl.multiple_of(me_tp * feats, LANES), feats)
        data = jnp.dot(
            pick[cap:], normed(mine), preferred_element_type=jnp.float32
        ).astype(jnp.bfloat16)
        for j in range(1, groups):
            rows_out[j, :, :feats] = data[(j - 1) * cap : j * cap]
            rows_out[j, :, feats:] = wdat[j * cap : (j + 1) * cap]

    with jax.named_scope("barrier"):
        pl.semaphore_wait(barrier, partners)
    sent = []

    def send(src, dst, ssem, rsem, ep, tp):
        copy = pltpu.make_async_remote_copy(
            src_ref=src, dst_ref=dst, send_sem=ssem, recv_sem=rsem,
            device_id={"ep": ep, "tp": tp}, device_id_type=MESH,
        )
        copy.start()
        sent.append(copy)

    def landed(dst, ssem, rsem):
        pltpu.make_async_remote_copy(
            src_ref=dst, dst_ref=dst, send_sem=ssem, recv_sem=rsem,
            device_id={"ep": me_ep, "tp": me_tp}, device_id_type=MESH,
        ).wait_recv()

    def lines(rank):
        return pl.ds(pl.multiple_of(rank * cap, cap), cap)

    def piece(j, core, yy, rank):
        return rows_in.at[j, core, yy, lines(rank)]

    def own(core, rank):
        return rows_own.at[core, lines(rank)]

    for j in range(1, groups):
        send(rows_out.at[j], piece(j, c, y, mate(j, p)), a_send.at[j],
             a_recv.at[j], rem(g - j, groups) * ranks + mate(j, p), twin())

    for core in range(CORES):
        cut = slice(core * side, (core + 1) * side)
        rows_own[core, lines(p), :side] = jnp.dot(
            pick[:cap], normed(cut), preferred_element_type=jnp.float32
        ).astype(jnp.bfloat16)
        rows_own[core, lines(p), side:] = wdat[:cap]

    near = sorted(range(1, ranks), key=lambda d: -(d // 2 + d % 2))
    hops = sorted(
        ((d, dy) for d in range(ranks) for dy in range(ys)),
        key=lambda h: (h != (0, 0), -(h[0] // 2 + h[0] % 2 + h[1])),
    )

    for d in near:
        send(own(c, p), own(c, p), s_send.at[d], s_recv.at[d], g * ranks + to(d), twin())

    def relay_own():
        for d in near:
            got = own(sib, of(d))
            landed(got, s_send.at[d], s_recv.at[d])
            send(got, got, q_send.at[d], q_recv.at[d], me_ep, twin())

    def spread(j):
        held = piece(j, sib, y, p)
        for d, dy in hops[1:]:
            send(held, held, b_send.at[j, d, dy], b_recv.at[j, d, dy], g * ranks + to(d), twin(dy))
        send(held, held, r_send.at[j, 0, 0], r_recv.at[j, 0, 0], me_ep, twin())

    def relay(j):
        for d, dy in hops[1:]:
            got = piece(j, c, rem(y - dy, ys), of(d))
            landed(got, b_send.at[j, d, dy], b_recv.at[j, d, dy])
            send(got, got, r_send.at[j, d, dy], r_recv.at[j, d, dy], me_ep, twin())

    def expand(j):
        gates = [jnp.zeros((ranks * cap, hidden), jnp.float32) for _ in range(experts)]
        ups = [jnp.zeros((ranks * cap, hidden), jnp.float32) for _ in range(experts)]

        def multiply(lhs, ks):
            for e in range(experts):
                gates[e] += jnp.dot(lhs, wg[e, ks, :], preferred_element_type=jnp.float32)
                ups[e] += jnp.dot(lhs, wu[e, ks, :], preferred_element_type=jnp.float32)

        if j == 0:
            for core in (sib, c):
                if core is c:
                    for d in near:
                        landed(own(c, of(d)), q_send.at[d], q_recv.at[d])
                multiply(rows_own[core, :, :side], pl.ds(pl.multiple_of(core * side, side), side))
            wrow = rows_own[sib, :, side:].astype(jnp.float32)
        else:
            landed(piece(j, c, y, p), r_send.at[j, 0, 0], r_recv.at[j, 0, 0])
            for core in (c, sib):
                if core is sib:
                    for d, dy in hops[1:]:
                        landed(piece(j, sib, rem(y - dy, ys), of(d)),
                               r_send.at[j, d, dy], r_recv.at[j, d, dy])
                for yy in range(ys):
                    ks = pl.ds(pl.multiple_of((yy * CORES + core) * feats, feats), feats)
                    multiply(rows_in[j, core, yy, :, :feats], ks)
            wrow = rows_in[j, c, 0, :, feats:].astype(jnp.float32)
        lanes = lax.broadcasted_iota(jnp.int32, wrow.shape, 1)
        for e in range(experts):
            w = jnp.sum(
                jnp.where(lax.rem(lanes, EPG) == p * experts + e, wrow, 0.0),
                axis=1, keepdims=True,
            )
            act = gates[e] / (1.0 + jnp.exp(-gates[e])) * ups[e] * w
            acts[j, c, y, :, e * hidden : (e + 1) * hidden] = act.astype(jnp.bfloat16)
        held = acts.at[j, c, y]
        for dy in range(1, ys):
            send(held, held, h_send.at[j, dy], h_recv.at[j, dy], me_ep, twin(dy))
        send(held, held, hr_send.at[j, 0], hr_recv.at[j, 0], me_ep, twin())

    def act_relay(j):
        for dy in range(1, ys):
            got = acts.at[j, sib, rem(y - dy, ys)]
            landed(got, h_send.at[j, dy], h_recv.at[j, dy])
            send(got, got, hr_send.at[j, dy], hr_recv.at[j, dy], me_ep, twin())

    def contract(j):
        total = jnp.zeros((ranks * cap, cols), jnp.float32)

        def multiply(core, yy, cut, total):
            ks = pl.ds(pl.multiple_of((yy * CORES + core) * hidden, hidden), hidden)
            for e in range(experts):
                total += jnp.dot(
                    acts[j, core, yy, :, e * hidden : (e + 1) * hidden],
                    wd[e, ks, cut], preferred_element_type=jnp.float32,
                )
            return total

        whole = slice(0, cols)
        total = multiply(c, y, whole, total)
        for dy in range(1, ys):
            total = multiply(sib, rem(y - dy, ys), whole, total)
        landed(acts.at[j, sib, y], hr_send.at[j, 0], hr_recv.at[j, 0])
        total = multiply(sib, y, whole, total)
        for dy in range(1, ys):
            landed(acts.at[j, c, rem(y - dy, ys)], hr_send.at[j, dy], hr_recv.at[j, dy])
        source = rem(g + j, groups) * ranks
        for b in range(SPLIT):
            cut = slice(b * block, (b + 1) * block)
            piece_total = total[:, cut]
            for dy in range(1, ys):
                piece_total = multiply(c, rem(y - dy, ys), cut, piece_total)
            parts[j, :, cut] = piece_total.astype(jnp.bfloat16)
            for d in reversed(range(ranks)):
                rows = lines(to(d))
                if j == 0 and d == 0:
                    back[0, p, :, cut] = parts[0, rows, cut]
                else:
                    send(parts.at[j, rows, cut], back.at[j, p, :, cut],
                         o_send.at[j, d, b], o_recv.at[j, d, b],
                         source + mate(j, to(d)), me_tp)

    for j in range(groups):
        if j + 1 < groups:
            with jax.named_scope(f"a_wait{j+1}"):
                landed(piece(j + 1, sib, y, p), a_send.at[j + 1], a_recv.at[j + 1])
            spread(j + 1)
        with jax.named_scope(f"relay{j}"):
            if j == 0:
                relay_own()
                loads[0].wait()
                loads[1].wait()
            else:
                relay(j)
        with jax.named_scope(f"expand{j}"):
            expand(j)
        if j:
            with jax.named_scope(f"act_relay{j-1}"):
                act_relay(j - 1)
            if j == 1:
                loads[2].wait()
            with jax.named_scope(f"contract{j-1}"):
                contract(j - 1)
    with jax.named_scope("act_relayL"):
        act_relay(groups - 1)
    if groups == 1:
        loads[2].wait()
    with jax.named_scope("contractL"):
        contract(groups - 1)

    sums = []
    for j in range(groups):
        with jax.named_scope(f"back{j}"):
            for b in range(SPLIT):
                for d in range(ranks):
                    if j or d:
                        landed(
                            back.at[j, shift(mate(j, p), d, -1), :, b * block : (b + 1) * block],
                            o_send.at[j, d, b], o_recv.at[j, d, b],
                        )
        total = back[j, 0].astype(jnp.float32)
        for k in range(1, ranks):
            total += back[j, k].astype(jnp.float32)
        sums.append(total.astype(jnp.bfloat16))
    with jax.named_scope("final"):
        place = (
            lax.broadcasted_iota(jnp.int32, (tokens, slots), 1) == slot(gcol, rank_col)
        ).astype(jnp.bfloat16)
        out_ref[...] = jnp.dot(
            place, jnp.concatenate(sums, axis=0), preferred_element_type=jnp.float32
        ).astype(jnp.bfloat16)
        for copy in sent:
            copy.wait_send()


def solution(mesh):
    ep_count, tp_count = mesh.shape["ep"], mesh.shape["tp"]

    def on_device(
        hidden_in, norm_gain, group_ids, inner_ids, group_prob, expert_prob, w_gate, w_up, w_down
    ):
        tokens = hidden_in.shape[0]
        experts, depth, hidden = w_gate.shape
        cols = w_down.shape[2]
        ranks, cap = EPG // experts, tokens // 2
        groups, ys = ep_count // ranks, tp_count // CORES
        feats, side = depth // tp_count, depth // CORES
        hbm = pl.BlockSpec(memory_space=pl.ANY)
        dma = pltpu.SemaphoreType.DMA
        small = (
            hidden_in, norm_gain.reshape(1, depth), group_ids.reshape(1, tokens), inner_ids.T,
            group_prob.reshape(1, tokens), expert_prob.T,
        )
        return pl.pallas_call(
            functools.partial(moe_kernel, ep_count, tp_count),
            out_shape=pltpu.VMEM((tokens, cols), jnp.bfloat16),
            in_specs=[hbm] * 9,
            out_specs=pl.BlockSpec(memory_space=pltpu.VMEM),
            scratch_shapes=[pltpu.VMEM(a.shape, a.dtype) for a in small] + [
                pltpu.VMEM(w_gate.shape, jnp.bfloat16),
                pltpu.VMEM(w_up.shape, jnp.bfloat16),
                pltpu.VMEM(w_down.shape, jnp.bfloat16),
                pltpu.VMEM((groups, cap, feats + LANES), jnp.bfloat16),
                pltpu.VMEM((CORES, ranks * cap, side + LANES), jnp.bfloat16),
                pltpu.VMEM((groups, CORES, ys, ranks * cap, feats + LANES), jnp.bfloat16),
                pltpu.VMEM((groups, CORES, ys, ranks * cap, experts * hidden), jnp.bfloat16),
                pltpu.VMEM((groups, ranks * cap, cols), jnp.bfloat16),
                pltpu.VMEM((groups, ranks, cap, cols), jnp.bfloat16),
                dma((len(small),)), dma((3,)),
                dma((groups,)), dma((groups,)),
                dma((ranks,)), dma((ranks,)),
                dma((ranks,)), dma((ranks,)),
                dma((groups, ranks, ys)), dma((groups, ranks, ys)),
                dma((groups, ranks, ys)), dma((groups, ranks, ys)),
                dma((groups, ys)), dma((groups, ys)),
                dma((groups, ys)), dma((groups, ys)),
                dma((groups, ranks, SPLIT)), dma((groups, ranks, SPLIT)),
            ],
            compiler_params=pltpu.CompilerParams(
                collective_id=0, has_side_effects=True, vmem_limit_bytes=56 * 1024 * 1024
            ),
        )(*small, w_gate, w_up, w_down)

    placed = (
        P("ep", None), P(), P("ep"), P("ep", None), P("ep"), P("ep", None),
        P("ep", None, "tp"), P("ep", None, "tp"), P("ep", None, "tp"),
    )
    return jax.shard_map(
        on_device, mesh=mesh, in_specs=placed, out_specs=P("ep", "tp"), check_vma=False
    )
```

```python
import functools

import jax
import jax.numpy as jnp
from jax import lax
from jax.experimental import pallas as pl
from jax.experimental.pallas import tpu as pltpu
from jax.sharding import PartitionSpec as P

EPG = 8
EPS = 1e-06
CORES = 2
LANES = 128
MESH = pl.DeviceIdType.MESH


def rem(value, count):
    return lax.rem(value + count, count)


def moe_kernel(
    ep_count, tp_count,
    hid_hbm, gain_hbm, grp_hbm, inner_hbm, gprob_hbm, eprob_hbm, wg_hbm, wu_hbm, wd_hbm,
    out_ref,
    hid_ref, gain_ref, grp_ref, inner_ref, gprob_ref, eprob_ref,
    wg, wu, wd, rows_out, rows_own, rows_in, acts, parts, back,
    i_sem, w_sem, a_send, a_recv, s_send, s_recv, q_send, q_recv, b_send, b_recv, r_send, r_recv,
    h_send, h_recv, hr_send, hr_recv, o_send, o_recv,
):
    experts, depth, hidden = wg.shape
    ranks = EPG // experts
    groups = ep_count // ranks
    ys = tp_count // CORES
    tokens = hid_ref.shape[0]
    cap = tokens // 2
    feats = depth // tp_count
    side = depth // CORES
    cols = wd.shape[2]

    me_ep, me_tp = lax.axis_index("ep"), lax.axis_index("tp")
    g, p = lax.div(me_ep, ranks), lax.rem(me_ep, ranks)
    y, c = lax.div(me_tp, CORES), lax.rem(me_tp, CORES)
    sib = 1 - c

    barrier = pltpu.get_barrier_semaphore()
    partners = 0

    def shift(rank, d, sign):
        return rem(lax.div(rank, 2) + sign * (d // 2), ranks // 2) * 2 + rem(
            lax.rem(rank, 2) + sign * (d % 2), 2
        )

    def to(d):
        return shift(p, d, 1)

    def of(d):
        return shift(p, d, -1)

    def mate(j, rank):
        return rank

    def twin(dy=0):
        return rem(y + dy, ys) * CORES + sib

    def greet(ep, tp):
        pl.semaphore_signal(
            barrier, inc=1, device_id={"ep": ep, "tp": tp}, device_id_type=MESH
        )

    for j in range(1, groups):
        greet(rem(g - j, groups) * ranks + mate(j, p), twin())
        partners += 1
    for d in range(ranks):
        for dy in range(ys):
            greet(g * ranks + to(d), twin(dy))
            partners += 1

    fetched = []
    for k, (src, dst) in enumerate((
        (hid_hbm, hid_ref), (gain_hbm, gain_ref), (grp_hbm, grp_ref), (inner_hbm, inner_ref),
        (gprob_hbm, gprob_ref), (eprob_hbm, eprob_ref),
    )):
        load = pltpu.make_async_copy(src, dst, i_sem.at[k])
        load.start()
        fetched.append(load)
    for load in fetched:
        load.wait()
    loads = []
    for k, (src, dst) in enumerate(((wg_hbm, wg), (wu_hbm, wu), (wd_hbm, wd))):
        load = pltpu.make_async_copy(src, dst, w_sem.at[k])
        load.start()
        loads.append(load)

    r0 = lax.broadcasted_iota(jnp.int32, (tokens, tokens), 0)
    r1 = lax.broadcasted_iota(jnp.int32, (tokens, tokens), 1)
    grow = jnp.broadcast_to(grp_ref[...], (tokens, tokens))
    gcol = jnp.sum(jnp.where(r0 == r1, grow, 0), axis=1, keepdims=True)
    same = gcol == grow
    rank_row = jnp.sum(jnp.where(same & (r0 < r1), 1, 0), axis=0, keepdims=True)
    rank_col = jnp.sum(jnp.where(same & (r1 < r0), 1, 0), axis=1, keepdims=True)

    def slot(group, rank):
        rel = g - group
        return jnp.where(rel < 0, rel + groups, rel) * cap + rank

    slots = groups * cap
    pick = (
        lax.broadcasted_iota(jnp.int32, (slots, tokens), 0) == slot(grp_ref[...], rank_row)
    ).astype(jnp.bfloat16)

    line = lax.broadcasted_iota(jnp.int32, (LANES, tokens), 0)
    inner, eprob, prob = inner_ref[...], eprob_ref[...], gprob_ref[...]
    weight = jnp.zeros((LANES, tokens), jnp.float32)
    for k in range(inner.shape[0]):
        hit = lax.rem(line, EPG) == inner[k : k + 1, :]
        weight += jnp.where(hit, prob * eprob[k : k + 1, :], 0.0)
    high = weight.astype(jnp.bfloat16).astype(jnp.float32)
    mid = (weight - high).astype(jnp.bfloat16).astype(jnp.float32)
    low = weight - high - mid
    part = lax.div(line, EPG)
    weight = jnp.where(
        part == 0, high, jnp.where(part == 1, mid, jnp.where(part == 2, low, 0.0))
    ).astype(jnp.bfloat16)
    wdat = lax.dot_general(
        pick, weight, (((1,), (1,)), ((), ())), preferred_element_type=jnp.float32
    ).astype(jnp.bfloat16)

    x = hid_ref[...].astype(jnp.float32)
    scale = lax.rsqrt(jnp.mean(x * x, axis=-1, keepdims=True) + EPS)

    def normed(cut):
        return (
            hid_ref[:, cut].astype(jnp.float32) * scale * gain_ref[:, cut]
        ).astype(jnp.bfloat16)

    if groups > 1:
        mine = pl.ds(pl.multiple_of(me_tp * feats, LANES), feats)
        data = jnp.dot(
            pick[cap:], normed(mine), preferred_element_type=jnp.float32
        ).astype(jnp.bfloat16)
        for j in range(1, groups):
            rows_out[j, :, :feats] = data[(j - 1) * cap : j * cap]
            rows_out[j, :, feats:] = wdat[j * cap : (j + 1) * cap]

    with jax.named_scope("barrier"):
        pl.semaphore_wait(barrier, partners)
    sent = []

    def send(src, dst, ssem, rsem, ep, tp):
        copy = pltpu.make_async_remote_copy(
            src_ref=src, dst_ref=dst, send_sem=ssem, recv_sem=rsem,
            device_id={"ep": ep, "tp": tp}, device_id_type=MESH,
        )
        copy.start()
        sent.append(copy)

    def landed(dst, ssem, rsem):
        pltpu.make_async_remote_copy(
            src_ref=dst, dst_ref=dst, send_sem=ssem, recv_sem=rsem,
            device_id={"ep": me_ep, "tp": me_tp}, device_id_type=MESH,
        ).wait_recv()

    def lines(rank):
        return pl.ds(pl.multiple_of(rank * cap, cap), cap)

    def piece(j, core, yy, rank):
        return rows_in.at[j, core, yy, lines(rank)]

    def own(core, rank):
        return rows_own.at[core, lines(rank)]

    for j in range(1, groups):
        send(rows_out.at[j], piece(j, c, y, mate(j, p)), a_send.at[j],
             a_recv.at[j], rem(g - j, groups) * ranks + mate(j, p), twin())

    for core in range(CORES):
        cut = slice(core * side, (core + 1) * side)
        rows_own[core, lines(p), :side] = jnp.dot(
            pick[:cap], normed(cut), preferred_element_type=jnp.float32
        ).astype(jnp.bfloat16)
        rows_own[core, lines(p), side:] = wdat[:cap]

    near = sorted(range(1, ranks), key=lambda d: -(d // 2 + d % 2))
    hops = sorted(
        ((d, dy) for d in range(ranks) for dy in range(ys)),
        key=lambda h: (h != (0, 0), -(h[0] // 2 + h[0] % 2 + h[1])),
    )

    for d in near:
        send(own(c, p), own(c, p), s_send.at[d], s_recv.at[d], g * ranks + to(d), twin())

    def relay_own():
        for d in near:
            got = own(sib, of(d))
            landed(got, s_send.at[d], s_recv.at[d])
            send(got, got, q_send.at[d], q_recv.at[d], me_ep, twin())

    def spread(j):
        held = piece(j, sib, y, p)
        for d, dy in hops[1:]:
            send(held, held, b_send.at[j, d, dy], b_recv.at[j, d, dy], g * ranks + to(d), twin(dy))
        send(held, held, r_send.at[j, 0, 0], r_recv.at[j, 0, 0], me_ep, twin())

    def relay(j):
        for d, dy in hops[1:]:
            got = piece(j, c, rem(y - dy, ys), of(d))
            landed(got, b_send.at[j, d, dy], b_recv.at[j, d, dy])
            send(got, got, r_send.at[j, d, dy], r_recv.at[j, d, dy], me_ep, twin())

    def expand(j):
        gates = [jnp.zeros((ranks * cap, hidden), jnp.float32) for _ in range(experts)]
        ups = [jnp.zeros((ranks * cap, hidden), jnp.float32) for _ in range(experts)]

        def multiply(lhs, ks):
            for e in range(experts):
                gates[e] += jnp.dot(lhs, wg[e, ks, :], preferred_element_type=jnp.float32)
                ups[e] += jnp.dot(lhs, wu[e, ks, :], preferred_element_type=jnp.float32)

        if j == 0:
            for core in (sib, c):
                if core is c:
                    for d in near:
                        landed(own(c, of(d)), q_send.at[d], q_recv.at[d])
                multiply(rows_own[core, :, :side], pl.ds(pl.multiple_of(core * side, side), side))
            wrow = rows_own[sib, :, side:].astype(jnp.float32)
        else:
            landed(piece(j, c, y, p), r_send.at[j, 0, 0], r_recv.at[j, 0, 0])
            for core in (c, sib):
                if core is sib:
                    for d, dy in hops[1:]:
                        landed(piece(j, sib, rem(y - dy, ys), of(d)),
                               r_send.at[j, d, dy], r_recv.at[j, d, dy])
                for yy in range(ys):
                    ks = pl.ds(pl.multiple_of((yy * CORES + core) * feats, feats), feats)
                    multiply(rows_in[j, core, yy, :, :feats], ks)
            wrow = rows_in[j, c, 0, :, feats:].astype(jnp.float32)
        lanes = lax.broadcasted_iota(jnp.int32, wrow.shape, 1)
        for e in range(experts):
            w = jnp.sum(
                jnp.where(lax.rem(lanes, EPG) == p * experts + e, wrow, 0.0),
                axis=1, keepdims=True,
            )
            act = gates[e] / (1.0 + jnp.exp(-gates[e])) * ups[e] * w
            acts[j, c, y, :, e * hidden : (e + 1) * hidden] = act.astype(jnp.bfloat16)
        held = acts.at[j, c, y]
        for dy in range(1, ys):
            send(held, held, h_send.at[j, dy], h_recv.at[j, dy], me_ep, twin(dy))
        send(held, held, hr_send.at[j, 0], hr_recv.at[j, 0], me_ep, twin())

    def act_relay(j):
        for dy in range(1, ys):
            got = acts.at[j, sib, rem(y - dy, ys)]
            landed(got, h_send.at[j, dy], h_recv.at[j, dy])
            send(got, got, hr_send.at[j, dy], hr_recv.at[j, dy], me_ep, twin())

    def contract(j):
        total = jnp.zeros((ranks * cap, cols), jnp.float32)

        def multiply(core, yy, cut, total):
            ks = pl.ds(pl.multiple_of((yy * CORES + core) * hidden, hidden), hidden)
            for e in range(experts):
                total += jnp.dot(
                    acts[j, core, yy, :, e * hidden : (e + 1) * hidden],
                    wd[e, ks, cut], preferred_element_type=jnp.float32,
                )
            return total

        whole = slice(0, cols)
        total = multiply(c, y, whole, total)
        for dy in range(1, ys):
            total = multiply(sib, rem(y - dy, ys), whole, total)
        landed(acts.at[j, sib, y], hr_send.at[j, 0], hr_recv.at[j, 0])
        total = multiply(sib, y, whole, total)
        for dy in range(1, ys):
            landed(acts.at[j, c, rem(y - dy, ys)], hr_send.at[j, dy], hr_recv.at[j, dy])
        for dy in range(1, ys):
            total = multiply(c, rem(y - dy, ys), whole, total)
        parts[j] = total.astype(jnp.bfloat16)
        if j == 0:
            for d in reversed(range(1, ranks)):
                send(parts.at[0, lines(to(d))], back.at[0, p], o_send.at[0, d], o_recv.at[0, p],
                     g * ranks + to(d), me_tp)
            back[0, p] = parts[0, lines(p), :]
            return
        for r in range(ranks):
            send(parts.at[j, lines(mate(j, r))], back.at[j, p], o_send.at[j, r], o_recv.at[j, p],
                 rem(g + j, groups) * ranks + r, me_tp)

    for j in range(groups):
        if j + 1 < groups:
            with jax.named_scope(f"a_wait{j+1}"):
                landed(piece(j + 1, sib, y, p), a_send.at[j + 1], a_recv.at[j + 1])
            spread(j + 1)
        with jax.named_scope(f"relay{j}"):
            if j == 0:
                relay_own()
                loads[0].wait()
                loads[1].wait()
            else:
                relay(j)
        with jax.named_scope(f"expand{j}"):
            expand(j)
        if j:
            with jax.named_scope(f"act_relay{j-1}"):
                act_relay(j - 1)
            if j == 1:
                loads[2].wait()
            with jax.named_scope(f"contract{j-1}"):
                contract(j - 1)
    with jax.named_scope("act_relayL"):
        act_relay(groups - 1)
    if groups == 1:
        loads[2].wait()
    with jax.named_scope("contractL"):
        contract(groups - 1)

    sums = []
    for j in range(groups):
        with jax.named_scope(f"back{j}"):
            for d in range(j == 0, ranks):
                k = of(d) if j == 0 else d
                landed(back.at[j, k], o_send.at[j, d], o_recv.at[j, k])
        total = back[j, 0].astype(jnp.float32)
        for k in range(1, ranks):
            total += back[j, k].astype(jnp.float32)
        sums.append(total.astype(jnp.bfloat16))
    with jax.named_scope("final"):
        place = (
            lax.broadcasted_iota(jnp.int32, (tokens, slots), 1) == slot(gcol, rank_col)
        ).astype(jnp.bfloat16)
        out_ref[...] = jnp.dot(
            place, jnp.concatenate(sums, axis=0), preferred_element_type=jnp.float32
        ).astype(jnp.bfloat16)
        for copy in sent:
            copy.wait_send()


def solution(mesh):
    ep_count, tp_count = mesh.shape["ep"], mesh.shape["tp"]

    def on_device(
        hidden_in, norm_gain, group_ids, inner_ids, group_prob, expert_prob, w_gate, w_up, w_down
    ):
        tokens = hidden_in.shape[0]
        experts, depth, hidden = w_gate.shape
        cols = w_down.shape[2]
        ranks, cap = EPG // experts, tokens // 2
        groups, ys = ep_count // ranks, tp_count // CORES
        feats, side = depth // tp_count, depth // CORES
        hbm = pl.BlockSpec(memory_space=pl.ANY)
        dma = pltpu.SemaphoreType.DMA
        small = (
            hidden_in, norm_gain.reshape(1, depth), group_ids.reshape(1, tokens), inner_ids.T,
            group_prob.reshape(1, tokens), expert_prob.T,
        )
        return pl.pallas_call(
            functools.partial(moe_kernel, ep_count, tp_count),
            out_shape=pltpu.VMEM((tokens, cols), jnp.bfloat16),
            in_specs=[hbm] * 9,
            out_specs=pl.BlockSpec(memory_space=pltpu.VMEM),
            scratch_shapes=[pltpu.VMEM(a.shape, a.dtype) for a in small] + [
                pltpu.VMEM(w_gate.shape, jnp.bfloat16),
                pltpu.VMEM(w_up.shape, jnp.bfloat16),
                pltpu.VMEM(w_down.shape, jnp.bfloat16),
                pltpu.VMEM((groups, cap, feats + LANES), jnp.bfloat16),
                pltpu.VMEM((CORES, ranks * cap, side + LANES), jnp.bfloat16),
                pltpu.VMEM((groups, CORES, ys, ranks * cap, feats + LANES), jnp.bfloat16),
                pltpu.VMEM((groups, CORES, ys, ranks * cap, experts * hidden), jnp.bfloat16),
                pltpu.VMEM((groups, ranks * cap, cols), jnp.bfloat16),
                pltpu.VMEM((groups, ranks, cap, cols), jnp.bfloat16),
                dma((len(small),)), dma((3,)),
                dma((groups,)), dma((groups,)),
                dma((ranks,)), dma((ranks,)),
                dma((ranks,)), dma((ranks,)),
                dma((groups, ranks, ys)), dma((groups, ranks, ys)),
                dma((groups, ranks, ys)), dma((groups, ranks, ys)),
                dma((groups, ys)), dma((groups, ys)),
                dma((groups, ys)), dma((groups, ys)),
                dma((groups, ranks)), dma((groups, ranks)),
            ],
            compiler_params=pltpu.CompilerParams(
                collective_id=0, has_side_effects=True, vmem_limit_bytes=56 * 1024 * 1024
            ),
        )(*small, w_gate, w_up, w_down)

    placed = (
        P("ep", None), P(), P("ep"), P("ep", None), P("ep"), P("ep", None),
        P("ep", None, "tp"), P("ep", None, "tp"), P("ep", None, "tp"),
    )
    return jax.shard_map(
        on_device, mesh=mesh, in_specs=placed, out_specs=P("ep", "tp"), check_vma=False
    )
```

```python
import functools

import jax
import jax.numpy as jnp
from jax import lax
from jax.experimental import pallas as pl
from jax.experimental.pallas import tpu as pltpu
from jax.sharding import PartitionSpec as P

EPG = 8
EPS = 1e-06
CORES = 2
LANES = 128
CHUNKS = 2
MESH = pl.DeviceIdType.MESH


def rem(value, count):
    return lax.rem(value + count, count)


def moe_kernel(
    ep_count, tp_count,
    hid_hbm, gain_hbm, grp_hbm, inner_hbm, gprob_hbm, eprob_hbm, wg_hbm, wu_hbm, wd_hbm,
    out_ref,
    hid_ref, gain_ref, grp_ref, inner_ref, gprob_ref, eprob_ref,
    wg, wu, wd, rows_out, rows_own, rows_in, acts, parts, back,
    i_sem, w_sem, step_send, a_recv, s_recv, q_recv, b_recv, r_recv, h_recv, hr_recv, o_recv,
):
    experts, depth, hidden = wg.shape
    ranks = EPG // experts
    groups = ep_count // ranks
    ys = tp_count // CORES
    tokens = hid_ref.shape[0]
    cap = tokens // 2
    feats = depth // tp_count
    side = depth // CORES
    cols = wd.shape[2]

    me_ep, me_tp = lax.axis_index("ep"), lax.axis_index("tp")
    g, p = lax.div(me_ep, ranks), lax.rem(me_ep, ranks)
    y, c = lax.div(me_tp, CORES), lax.rem(me_tp, CORES)
    sib = 1 - c

    barrier = pltpu.get_barrier_semaphore()
    partners = 0

    def shift(rank, d, sign):
        return rem(lax.div(rank, 2) + sign * (d // 2), ranks // 2) * 2 + rem(
            lax.rem(rank, 2) + sign * (d % 2), 2
        )

    def to(d):
        return shift(p, d, 1)

    def of(d):
        return shift(p, d, -1)

    def twin(dy=0):
        return (lax.rem(y + dy, ys) if dy else y) * CORES + sib

    def greet(ep, tp):
        pl.semaphore_signal(
            barrier, inc=1, device_id={"ep": ep, "tp": tp}, device_id_type=MESH
        )

    for j in range(1, groups):
        greet(rem(g - j, groups) * ranks + p, twin())
        partners += 1
    for d in range(ranks):
        for dy in range(ys):
            greet(g * ranks + to(d), twin(dy))
            partners += 1

    fetched = []
    for k, (src, dst) in enumerate((
        (hid_hbm, hid_ref), (gain_hbm, gain_ref), (grp_hbm, grp_ref), (inner_hbm, inner_ref),
        (gprob_hbm, gprob_ref), (eprob_hbm, eprob_ref),
    )):
        load = pltpu.make_async_copy(src, dst, i_sem.at[k])
        load.start()
        fetched.append(load)
    for load in fetched:
        load.wait()
    loads = []
    for k, (src, dst) in enumerate(((wg_hbm, wg), (wu_hbm, wu), (wd_hbm, wd))):
        load = pltpu.make_async_copy(src, dst, w_sem.at[k])
        load.start()
        loads.append(load)

    r0 = lax.broadcasted_iota(jnp.int32, (tokens, tokens), 0)
    r1 = lax.broadcasted_iota(jnp.int32, (tokens, tokens), 1)
    grow = jnp.broadcast_to(grp_ref[...], (tokens, tokens))
    gcol = jnp.sum(jnp.where(r0 == r1, grow, 0), axis=1, keepdims=True)
    same = gcol == grow
    rank_row = jnp.sum(jnp.where(same & (r0 < r1), 1, 0), axis=0, keepdims=True)
    rank_col = jnp.sum(jnp.where(same & (r1 < r0), 1, 0), axis=1, keepdims=True)

    def slot(group, rank):
        rel = g - group
        return jnp.where(rel < 0, rel + groups, rel) * cap + rank

    slots = groups * cap
    pick = (
        lax.broadcasted_iota(jnp.int32, (slots, tokens), 0) == slot(grp_ref[...], rank_row)
    ).astype(jnp.bfloat16)

    line = lax.broadcasted_iota(jnp.int32, (LANES, tokens), 0)
    inner, eprob, prob = inner_ref[...], eprob_ref[...], gprob_ref[...]
    weight = jnp.zeros((LANES, tokens), jnp.float32)
    for k in range(inner.shape[0]):
        hit = lax.rem(line, EPG) == inner[k : k + 1, :]
        weight += jnp.where(hit, prob * eprob[k : k + 1, :], 0.0)
    high = weight.astype(jnp.bfloat16).astype(jnp.float32)
    mid = (weight - high).astype(jnp.bfloat16).astype(jnp.float32)
    low = weight - high - mid
    part = lax.div(line, EPG)
    weight = jnp.where(
        part == 0, high, jnp.where(part == 1, mid, jnp.where(part == 2, low, 0.0))
    ).astype(jnp.bfloat16)
    wdat = lax.dot_general(
        pick, weight, (((1,), (1,)), ((), ())), preferred_element_type=jnp.float32
    ).astype(jnp.bfloat16)

    x = hid_ref[...].astype(jnp.float32)
    scale = lax.rsqrt(jnp.mean(x * x, axis=-1, keepdims=True) + EPS)

    def normed(cut):
        return (
            hid_ref[:, cut].astype(jnp.float32) * scale * gain_ref[:, cut]
        ).astype(jnp.bfloat16)

    if groups > 1:
        mine = pl.ds(pl.multiple_of(me_tp * feats, LANES), feats)
        data = jnp.dot(
            pick[cap:], normed(mine), preferred_element_type=jnp.float32
        ).astype(jnp.bfloat16)
        for j in range(1, groups):
            rows_out[j - 1, :, :feats] = data[(j - 1) * cap : j * cap]
            rows_out[j - 1, :, feats:] = wdat[j * cap : (j + 1) * cap]

    with jax.named_scope("barrier"):
        pl.semaphore_wait(barrier, partners)
    pending = {}

    def bulk(size):
        return wg.at[0, : size // (hidden * 2)]

    def send(src, dst, ssem, rsem, ep, tp, key):
        pltpu.make_async_remote_copy(
            src_ref=src, dst_ref=dst, send_sem=ssem, recv_sem=rsem,
            device_id={"ep": ep, "tp": tp}, device_id_type=MESH,
        ).start()
        size = 2
        for extent in src.shape:
            size *= extent
        pending[key] = (ssem, pending.get(key, (ssem, 0))[1] + size)

    def wait_of(dst, sem):
        return pltpu.make_async_remote_copy(
            src_ref=dst, dst_ref=dst, send_sem=sem, recv_sem=sem,
            device_id={"ep": me_ep, "tp": me_tp}, device_id_type=MESH,
        )

    def landed(dst, sem):
        wait_of(dst, sem).wait_recv()

    def lines(rank):
        start = rank * cap
        return pl.ds(start if isinstance(rank, int) else pl.multiple_of(start, cap), cap)

    def piece(j, core, yy, rank):
        return rows_in.at[j, core, yy, lines(rank)]

    def own(core, rank):
        return rows_own.at[core, lines(rank)]

    for j in range(1, groups):
        send(rows_out.at[j - 1], piece(j, c, y, p), step_send.at[j],
             a_recv.at[j - 1], rem(g - j, groups) * ranks + p, twin(), j)

    for core in range(CORES):
        cut = slice(core * side, (core + 1) * side)
        rows_own[core, lines(p), :side] = jnp.dot(
            pick[:cap], normed(cut), preferred_element_type=jnp.float32
        ).astype(jnp.bfloat16)
        rows_own[core, lines(p), side:] = wdat[:cap]

    near = sorted(range(1, ranks), key=lambda d: -(d // 2 + d % 2))
    hops = [
        (d, dy) for dy in reversed(range(ys)) for d in near + [0] if d or dy
    ]

    for d in near:
        send(own(c, p), own(c, p), step_send.at[0], s_recv.at[d - 1], g * ranks + to(d), twin(), 0)

    def relay_own():
        for d in near:
            got = own(sib, of(d))
            landed(got, s_recv.at[d - 1])
            send(got, got, step_send.at[0], q_recv.at[0], me_ep, twin(), 0)

    def spread(j):
        held = piece(j, sib, y, p)
        bare = held.at[:, :feats]
        for i, (d, dy) in enumerate(hops):
            part = bare if dy else held
            send(part, part, step_send.at[j], b_recv.at[j - 1, i], g * ranks + to(d), twin(dy), j)
        send(bare, bare, step_send.at[j], r_recv.at[j - 1, 0], me_ep, twin(), j)

    def chunks(j):
        count = 1 if j == 0 else CHUNKS
        size = ranks * cap // count
        return [slice(k * size, (k + 1) * size) for k in range(count)]

    def expand(j):
        gates = [jnp.zeros((ranks * cap, hidden), jnp.float32) for _ in range(experts)]
        ups = [jnp.zeros((ranks * cap, hidden), jnp.float32) for _ in range(experts)]

        def multiply(load, ks):
            lhs = load(slice(None))
            for e in range(experts):
                gates[e] += jnp.dot(lhs, wg[e, ks, :], preferred_element_type=jnp.float32)
                ups[e] += jnp.dot(lhs, wu[e, ks, :], preferred_element_type=jnp.float32)

        def finish(load, ks, wrow):
            lanes = lax.broadcasted_iota(jnp.int32, wrow.shape, 1)
            scales = [
                jnp.sum(
                    jnp.where(lax.rem(lanes, EPG) == p * experts + e, wrow, 0.0),
                    axis=1, keepdims=True,
                ) for e in range(experts)
            ]
            multiply(load, ks)
            for k, rows in enumerate(chunks(j)):
                for e in range(experts):
                    gate, up = gates[e][rows], ups[e][rows]
                    act = gate / (1.0 + jnp.exp(-gate)) * up * scales[e][rows]
                    acts[j, c, y, rows, e * hidden : (e + 1) * hidden] = act.astype(jnp.bfloat16)
                held = acts.at[j, c, y, rows]
                for dy in range(1, ys):
                    send(held, held, step_send.at[j], h_recv.at[j, k, dy - 1], me_ep, twin(dy), j)
                send(held, held, step_send.at[j], hr_recv.at[j, k, 0], me_ep, twin(), j)

        if j == 0:
            def half(core):
                return (
                    lambda rows: rows_own[core, rows, :side],
                    pl.ds(pl.multiple_of(core * side, side), side),
                )

            multiply(*half(sib))
            landed(rows_own.at[c, : (ranks - 1) * cap], q_recv.at[0])
            finish(*half(c), rows_own[sib, :, side:].astype(jnp.float32))
            return

        def quarter(core, dy):
            yy = rem(y - dy, ys)
            return (
                lambda rows: rows_in[j, core, yy, rows, :feats],
                pl.ds(pl.multiple_of((yy * CORES + core) * feats, feats), feats),
            )

        for dy in reversed(range(ys)):
            for i, (d, hop) in enumerate(hops):
                if hop == dy:
                    got = piece(j, c, rem(y - dy, ys), of(d))
                    landed(got.at[:, :feats] if dy else got, b_recv.at[j - 1, i])
                    got = got.at[:, :feats]
                    send(got, got, step_send.at[j], r_recv.at[j - 1, 1 + dy], me_ep, twin(), j)
            if dy == 0:
                landed(piece(j, c, y, p).at[:, :feats], r_recv.at[j - 1, 0])
            multiply(*quarter(c, dy))
        rows_in[j, c, y, lines(p), feats:] = rows_in[j, sib, y, lines(p), feats:]
        wrow = rows_in[j, c, y, :, feats:].astype(jnp.float32)
        for dy in reversed(range(ys)):
            landed(bulk((ranks - (dy == 0)) * cap * feats * 2), r_recv.at[j - 1, 1 + dy])
            if dy:
                multiply(*quarter(sib, dy))
            else:
                finish(*quarter(sib, dy), wrow)

    def collect(j):
        landed(parts.at[j, : (ranks - 1 if j == 0 else ranks) * cap], o_recv.at[j])

    def contract(j):
        def multiply(core, dy, rows, total):
            yy = rem(y - dy, ys)
            ks = pl.ds(pl.multiple_of((yy * CORES + core) * hidden, hidden), hidden)
            for e in range(experts):
                total += jnp.dot(
                    acts[j, core, yy, rows, e * hidden : (e + 1) * hidden],
                    wd[e, ks, :], preferred_element_type=jnp.float32,
                )
            return total

        cuts = chunks(j)
        whole = multiply(c, 0, slice(None), jnp.zeros((ranks * cap, cols), jnp.float32))
        for k in range(len(cuts)):
            landed(acts.at[j, sib, y, cuts[k]], hr_recv.at[j, k, 0])
        whole = multiply(sib, 0, slice(None), whole)

        def relay(k):
            for dy in range(1, ys):
                got = acts.at[j, sib, rem(y - dy, ys), cuts[k]]
                landed(got, h_recv.at[j, k, dy - 1])
                send(got, got, step_send.at[j], hr_recv.at[j, k, dy], me_ep, twin(), j)

        relay(0)
        for k, rows in enumerate(cuts):
            if k:
                collect(j - 1)
            total = whole[rows]
            for dy in range(1, ys):
                total = multiply(sib, dy, rows, total)
            if k + 1 < len(cuts):
                relay(k + 1)
            for dy in range(1, ys):
                landed(acts.at[j, c, rem(y - dy, ys), rows], hr_recv.at[j, k, dy])
                total = multiply(c, dy, rows, total)
            parts[j, rows] = total.astype(jnp.bfloat16)
            if j == 0:
                for d in near:
                    send(parts.at[0, lines(to(d))], back.at[0, p], step_send.at[0], o_recv.at[0],
                         g * ranks + to(d), me_tp, 0)
                back[0, p] = parts[0, lines(p), :]
                continue
            for r in range(rows.start // cap, rows.stop // cap):
                send(parts.at[j, lines(r)], back.at[j, p], step_send.at[j], o_recv.at[j],
                     lax.rem(g + j, groups) * ranks + r, me_tp, j)

    for j in range(groups):
        if j + 1 < groups:
            with jax.named_scope(f"a_wait{j+1}"):
                landed(piece(j + 1, sib, y, p), a_recv.at[j])
            spread(j + 1)
        if j == 0:
            with jax.named_scope("relay0"):
                relay_own()
            loads[0].wait()
            loads[1].wait()
        with jax.named_scope(f"expand{j}"):
            expand(j)
        if j:
            if j == 1:
                loads[2].wait()
            with jax.named_scope(f"contract{j-1}"):
                contract(j - 1)
    if groups == 1:
        loads[2].wait()
    with jax.named_scope("contractL"):
        contract(groups - 1)

    with jax.named_scope("back1"):
        collect(groups - 1)
    with jax.named_scope("final"):
        spot = lax.broadcasted_iota(jnp.int32, (tokens, ranks * slots), 1)
        spot = lax.div(spot, ranks * cap) * cap + lax.rem(spot, cap)
        place = (spot == slot(gcol, rank_col)).astype(jnp.bfloat16)
        out_ref[...] = jnp.dot(
            place, back[...].reshape(ranks * slots, cols), preferred_element_type=jnp.float32
        ).astype(jnp.bfloat16)
        for sem, size in pending.values():
            wait_of(bulk(size), sem).wait_send()


def solution(mesh):
    ep_count, tp_count = mesh.shape["ep"], mesh.shape["tp"]

    def on_device(
        hidden_in, norm_gain, group_ids, inner_ids, group_prob, expert_prob, w_gate, w_up, w_down
    ):
        tokens = hidden_in.shape[0]
        experts, depth, hidden = w_gate.shape
        cols = w_down.shape[2]
        ranks, cap = EPG // experts, tokens // 2
        groups, ys = ep_count // ranks, tp_count // CORES
        feats, side = depth // tp_count, depth // CORES
        others = max(groups - 1, 1)
        hbm = pl.BlockSpec(memory_space=pl.ANY)
        dma = pltpu.SemaphoreType.DMA
        small = (
            hidden_in, norm_gain.reshape(1, depth), group_ids.reshape(1, tokens), inner_ids.T,
            group_prob.reshape(1, tokens), expert_prob.T,
        )
        return pl.pallas_call(
            functools.partial(moe_kernel, ep_count, tp_count),
            out_shape=pltpu.VMEM((tokens, cols), jnp.bfloat16),
            in_specs=[hbm] * 9,
            out_specs=pl.BlockSpec(memory_space=pltpu.VMEM),
            scratch_shapes=[pltpu.VMEM(a.shape, a.dtype) for a in small] + [
                pltpu.VMEM(w_gate.shape, jnp.bfloat16),
                pltpu.VMEM(w_up.shape, jnp.bfloat16),
                pltpu.VMEM(w_down.shape, jnp.bfloat16),
                pltpu.VMEM((others, cap, feats + LANES), jnp.bfloat16),
                pltpu.VMEM((CORES, ranks * cap, side + LANES), jnp.bfloat16),
                pltpu.VMEM((groups, CORES, ys, ranks * cap, feats + LANES), jnp.bfloat16),
                pltpu.VMEM((groups, CORES, ys, ranks * cap, experts * hidden), jnp.bfloat16),
                pltpu.VMEM((groups, ranks * cap, cols), jnp.bfloat16),
                pltpu.VMEM((groups, ranks, cap, cols), jnp.bfloat16),
                dma((len(small),)), dma((3,)), dma((groups,)),
                dma((others,)), dma((ranks - 1,)), dma((1,)),
                dma((others, ranks * ys - 1)), dma((others, ys + 1)),
                dma((groups, CHUNKS, ys - 1)), dma((groups, CHUNKS, ys)), dma((groups,)),
            ],
            compiler_params=pltpu.CompilerParams(
                collective_id=0, has_side_effects=True, vmem_limit_bytes=56 * 1024 * 1024
            ),
        )(*small, w_gate, w_up, w_down)

    placed = (
        P("ep", None), P(), P("ep"), P("ep", None), P("ep"), P("ep", None),
        P("ep", None, "tp"), P("ep", None, "tp"), P("ep", None, "tp"),
    )
    return jax.shard_map(
        on_device, mesh=mesh, in_specs=placed, out_specs=P("ep", "tp"), check_vma=False
    )
```

```python
import functools

import jax
import jax.numpy as jnp
from jax import lax
from jax.experimental import pallas as pl
from jax.experimental.pallas import tpu as pltpu
from jax.sharding import PartitionSpec as P

EPG = 8
EPS = 1e-06
CORES = 2
LANES = 128
CHUNKS = 2
MESH = pl.DeviceIdType.MESH


def rem(value, count):
    return lax.rem(value + count, count)


def moe_kernel(
    ep_count, tp_count,
    hid_hbm, gain_hbm, grp_hbm, inner_hbm, gprob_hbm, eprob_hbm, wg_hbm, wu_hbm, wd_hbm,
    out_ref,
    hid_ref, gain_ref, grp_ref, inner_ref, gprob_ref, eprob_ref,
    wg, wu, wd, rows_out, rows_own, rows_in, acts, parts, back,
    i_sem, w_sem, step_send, a_recv, s_recv, q_recv, b_recv, r_recv, h_recv, hr_recv, g_recv, o_recv,
):
    experts, depth, hidden = wg.shape
    ranks = EPG // experts
    groups = ep_count // ranks
    ys = tp_count // CORES
    tokens = hid_ref.shape[0]
    cap = tokens // 2
    feats = depth // tp_count
    side = depth // CORES
    cols = wd.shape[2]

    me_ep, me_tp = lax.axis_index("ep"), lax.axis_index("tp")
    g, p = lax.div(me_ep, ranks), lax.rem(me_ep, ranks)
    y, c = lax.div(me_tp, CORES), lax.rem(me_tp, CORES)
    sib = 1 - c

    barrier = pltpu.get_barrier_semaphore()
    partners = 0

    def shift(rank, d, sign):
        return rem(lax.div(rank, 2) + sign * (d // 2), ranks // 2) * 2 + rem(
            lax.rem(rank, 2) + sign * (d % 2), 2
        )

    def to(d):
        return shift(p, d, 1)

    def of(d):
        return shift(p, d, -1)

    def twin(dy=0):
        return (lax.rem(y + dy, ys) if dy else y) * CORES + sib

    def greet(ep, tp):
        pl.semaphore_signal(
            barrier, inc=1, device_id={"ep": ep, "tp": tp}, device_id_type=MESH
        )

    for j in range(1, groups):
        greet(rem(g - j, groups) * ranks + p, twin())
        partners += 1
    for d in range(ranks):
        for dy in range(ys):
            greet(g * ranks + to(d), twin(dy))
            partners += 1
    for dy in range(1, ys):
        greet(me_ep, lax.rem(y + dy, ys) * CORES + c)
        partners += 1

    fetched = []
    for k, (src, dst) in enumerate((
        (hid_hbm, hid_ref), (gain_hbm, gain_ref), (grp_hbm, grp_ref), (inner_hbm, inner_ref),
        (gprob_hbm, gprob_ref), (eprob_hbm, eprob_ref),
    )):
        load = pltpu.make_async_copy(src, dst, i_sem.at[k])
        load.start()
        fetched.append(load)
    for load in fetched:
        load.wait()
    loads = []
    for k, (src, dst) in enumerate(((wg_hbm, wg), (wu_hbm, wu), (wd_hbm, wd))):
        load = pltpu.make_async_copy(src, dst, w_sem.at[k])
        load.start()
        loads.append(load)

    r0 = lax.broadcasted_iota(jnp.int32, (tokens, tokens), 0)
    r1 = lax.broadcasted_iota(jnp.int32, (tokens, tokens), 1)
    grow = jnp.broadcast_to(grp_ref[...], (tokens, tokens))
    gcol = jnp.sum(jnp.where(r0 == r1, grow, 0), axis=1, keepdims=True)
    same = gcol == grow
    rank_row = jnp.sum(jnp.where(same & (r0 < r1), 1, 0), axis=0, keepdims=True)
    rank_col = jnp.sum(jnp.where(same & (r1 < r0), 1, 0), axis=1, keepdims=True)

    def slot(group, rank):
        rel = g - group
        return jnp.where(rel < 0, rel + groups, rel) * cap + rank

    slots = groups * cap
    pick = (
        lax.broadcasted_iota(jnp.int32, (slots, tokens), 0) == slot(grp_ref[...], rank_row)
    ).astype(jnp.bfloat16)

    line = lax.broadcasted_iota(jnp.int32, (LANES, tokens), 0)
    inner, eprob, prob = inner_ref[...], eprob_ref[...], gprob_ref[...]
    weight = jnp.zeros((LANES, tokens), jnp.float32)
    for k in range(inner.shape[0]):
        hit = lax.rem(line, EPG) == inner[k : k + 1, :]
        weight += jnp.where(hit, prob * eprob[k : k + 1, :], 0.0)
    high = weight.astype(jnp.bfloat16).astype(jnp.float32)
    mid = (weight - high).astype(jnp.bfloat16).astype(jnp.float32)
    low = weight - high - mid
    part = lax.div(line, EPG)
    weight = jnp.where(
        part == 0, high, jnp.where(part == 1, mid, jnp.where(part == 2, low, 0.0))
    ).astype(jnp.bfloat16)
    wdat = lax.dot_general(
        pick, weight, (((1,), (1,)), ((), ())), preferred_element_type=jnp.float32
    ).astype(jnp.bfloat16)

    x = hid_ref[...].astype(jnp.float32)
    scale = lax.rsqrt(jnp.mean(x * x, axis=-1, keepdims=True) + EPS)

    def normed(cut):
        return (
            hid_ref[:, cut].astype(jnp.float32) * scale * gain_ref[:, cut]
        ).astype(jnp.bfloat16)

    if groups > 1:
        mine = pl.ds(pl.multiple_of(me_tp * feats, LANES), feats)
        data = jnp.dot(
            pick[cap:], normed(mine), preferred_element_type=jnp.float32
        ).astype(jnp.bfloat16)
        for j in range(1, groups):
            rows_out[j - 1, :, :feats] = data[(j - 1) * cap : j * cap]
            rows_out[j - 1, :, feats:] = wdat[j * cap : (j + 1) * cap]

    with jax.named_scope("barrier"):
        pl.semaphore_wait(barrier, partners)
    pending = {}

    def bulk(size):
        return wg.at[0, : size // (hidden * 2)]

    def send(src, dst, ssem, rsem, ep, tp, key):
        pltpu.make_async_remote_copy(
            src_ref=src, dst_ref=dst, send_sem=ssem, recv_sem=rsem,
            device_id={"ep": ep, "tp": tp}, device_id_type=MESH,
        ).start()
        size = 2
        for extent in src.shape:
            size *= extent
        pending[key] = (ssem, pending.get(key, (ssem, 0))[1] + size)

    def wait_of(dst, sem):
        return pltpu.make_async_remote_copy(
            src_ref=dst, dst_ref=dst, send_sem=sem, recv_sem=sem,
            device_id={"ep": me_ep, "tp": me_tp}, device_id_type=MESH,
        )

    def landed(dst, sem):
        wait_of(dst, sem).wait_recv()

    def lines(rank):
        start = rank * cap
        return pl.ds(start if isinstance(rank, int) else pl.multiple_of(start, cap), cap)

    def piece(j, core, yy, rank):
        return rows_in.at[j, core, yy, lines(rank)]

    def own(core, rank):
        return rows_own.at[core, lines(rank)]

    for j in range(1, groups):
        send(rows_out.at[j - 1], piece(j, c, y, p), step_send.at[j],
             a_recv.at[j - 1], rem(g - j, groups) * ranks + p, twin(), j)

    for core in range(CORES):
        cut = slice(core * side, (core + 1) * side)
        rows_own[core, lines(p), :side] = jnp.dot(
            pick[:cap], normed(cut), preferred_element_type=jnp.float32
        ).astype(jnp.bfloat16)
        rows_own[core, lines(p), side:] = wdat[:cap]

    near = sorted(range(1, ranks), key=lambda d: -(d // 2 + d % 2))
    hops = [
        (d, dy) for dy in reversed(range(ys)) for d in near + [0] if d or dy
    ]

    for d in near:
        send(own(c, p), own(c, p), step_send.at[0], s_recv.at[d - 1], g * ranks + to(d), twin(), 0)

    def relay_own():
        for d in near:
            got = own(sib, of(d))
            landed(got, s_recv.at[d - 1])
            send(got, got, step_send.at[0], q_recv.at[0], me_ep, twin(), 0)

    def spread(j):
        held = piece(j, sib, y, p)
        bare = held.at[:, :feats]
        for i, (d, dy) in enumerate(hops):
            part = bare if dy else held
            send(part, part, step_send.at[j], b_recv.at[j - 1, i], g * ranks + to(d), twin(dy), j)
        send(bare, bare, step_send.at[j], r_recv.at[j - 1, 0], me_ep, twin(), j)

    def chunks(j):
        count = 1 if j == 0 else CHUNKS
        size = ranks * cap // count
        return [slice(k * size, (k + 1) * size) for k in range(count)]

    def expand(j):
        gates = [jnp.zeros((ranks * cap, hidden), jnp.float32) for _ in range(experts)]
        ups = [jnp.zeros((ranks * cap, hidden), jnp.float32) for _ in range(experts)]

        def multiply(load, ks):
            lhs = load(slice(None))
            for e in range(experts):
                gates[e] += jnp.dot(lhs, wg[e, ks, :], preferred_element_type=jnp.float32)
                ups[e] += jnp.dot(lhs, wu[e, ks, :], preferred_element_type=jnp.float32)

        def finish(load, ks, wrow):
            lanes = lax.broadcasted_iota(jnp.int32, wrow.shape, 1)
            scales = [
                jnp.sum(
                    jnp.where(lax.rem(lanes, EPG) == p * experts + e, wrow, 0.0),
                    axis=1, keepdims=True,
                ) for e in range(experts)
            ]
            multiply(load, ks)
            for k, rows in enumerate(chunks(j)):
                for e in range(experts):
                    gate, up = gates[e][rows], ups[e][rows]
                    act = gate / (1.0 + jnp.exp(-gate)) * up * scales[e][rows]
                    acts[j, c, y, rows, e * hidden : (e + 1) * hidden] = act.astype(jnp.bfloat16)
                held = acts.at[j, c, y, rows]
                for dy in range(1, ys):
                    if j == 0:
                        send(held, held, step_send.at[j], h_recv.at[dy - 1], me_ep, twin(dy), j)
                        continue
                    for core in reversed(range(CORES)):
                        send(held, held, step_send.at[j], g_recv.at[j - 1, k, c, dy - 1], me_ep,
                             lax.rem(y + dy, ys) * CORES + core, j)
                send(held, held, step_send.at[j], hr_recv.at[j, k, 0], me_ep, twin(), j)

        if j == 0:
            def half(core):
                return (
                    lambda rows: rows_own[core, rows, :side],
                    pl.ds(pl.multiple_of(core * side, side), side),
                )

            multiply(*half(sib))
            landed(rows_own.at[c, : (ranks - 1) * cap], q_recv.at[0])
            finish(*half(c), rows_own[sib, :, side:].astype(jnp.float32))
            return

        def quarter(core, dy):
            yy = rem(y - dy, ys)
            return (
                lambda rows: rows_in[j, core, yy, rows, :feats],
                pl.ds(pl.multiple_of((yy * CORES + core) * feats, feats), feats),
            )

        for dy in reversed(range(ys)):
            for i, (d, hop) in enumerate(hops):
                if hop == dy:
                    got = piece(j, c, rem(y - dy, ys), of(d))
                    landed(got.at[:, :feats] if dy else got, b_recv.at[j - 1, i])
                    got = got.at[:, :feats]
                    send(got, got, step_send.at[j], r_recv.at[j - 1, 1 + dy], me_ep, twin(), j)
            if dy == 0:
                landed(piece(j, c, y, p).at[:, :feats], r_recv.at[j - 1, 0])
            multiply(*quarter(c, dy))
        rows_in[j, c, y, lines(p), feats:] = rows_in[j, sib, y, lines(p), feats:]
        wrow = rows_in[j, c, y, :, feats:].astype(jnp.float32)
        for dy in reversed(range(ys)):
            landed(bulk((ranks - (dy == 0)) * cap * feats * 2), r_recv.at[j - 1, 1 + dy])
            if dy:
                multiply(*quarter(sib, dy))
            else:
                finish(*quarter(sib, dy), wrow)

    def collect(j):
        landed(parts.at[j, : (ranks - 1 if j == 0 else ranks) * cap], o_recv.at[j])

    def contract(j):
        def multiply(core, dy, rows, total):
            yy = rem(y - dy, ys)
            ks = pl.ds(pl.multiple_of((yy * CORES + core) * hidden, hidden), hidden)
            for e in range(experts):
                total += jnp.dot(
                    acts[j, core, yy, rows, e * hidden : (e + 1) * hidden],
                    wd[e, ks, :], preferred_element_type=jnp.float32,
                )
            return total

        cuts = chunks(j)
        whole = multiply(c, 0, slice(None), jnp.zeros((ranks * cap, cols), jnp.float32))
        for k in range(len(cuts)):
            landed(acts.at[j, sib, y, cuts[k]], hr_recv.at[j, k, 0])
        whole = multiply(sib, 0, slice(None), whole)

        if j == 0:
            for dy in range(1, ys):
                got = acts.at[0, sib, rem(y - dy, ys)]
                landed(got, h_recv.at[dy - 1])
                send(got, got, step_send.at[0], hr_recv.at[0, 0, dy], me_ep, twin(), 0)
        for k, rows in enumerate(cuts):
            total = whole[rows]
            for dy in range(1, ys):
                for core in (sib, c):
                    got = acts.at[j, core, rem(y - dy, ys), rows]
                    if j:
                        landed(got, g_recv.at[j - 1, k, core, dy - 1])
                    elif core is c:
                        landed(got, hr_recv.at[0, 0, dy])
                    total = multiply(core, dy, rows, total)
            parts[j, rows] = total.astype(jnp.bfloat16)
            if j == 0:
                for d in near:
                    send(parts.at[0, lines(to(d))], back.at[0, p], step_send.at[0], o_recv.at[0],
                         g * ranks + to(d), me_tp, 0)
                back[0, p] = parts[0, lines(p), :]
                continue
            if k:
                collect(j - 1)
            for r in range(rows.start // cap, rows.stop // cap):
                send(parts.at[j, lines(r)], back.at[j, p], step_send.at[j], o_recv.at[j],
                     lax.rem(g + j, groups) * ranks + r, me_tp, j)

    for j in range(groups):
        if j + 1 < groups:
            with jax.named_scope(f"a_wait{j+1}"):
                landed(piece(j + 1, sib, y, p), a_recv.at[j])
            spread(j + 1)
        if j == 0:
            with jax.named_scope("relay0"):
                relay_own()
            loads[0].wait()
            loads[1].wait()
        with jax.named_scope(f"expand{j}"):
            expand(j)
        if j:
            if j == 1:
                loads[2].wait()
            with jax.named_scope(f"contract{j-1}"):
                contract(j - 1)
    if groups == 1:
        loads[2].wait()
    with jax.named_scope("contractL"):
        contract(groups - 1)

    with jax.named_scope("back1"):
        collect(groups - 1)
    with jax.named_scope("final"):
        spot = lax.broadcasted_iota(jnp.int32, (tokens, ranks * slots), 1)
        spot = lax.div(spot, ranks * cap) * cap + lax.rem(spot, cap)
        place = (spot == slot(gcol, rank_col)).astype(jnp.bfloat16)
        out_ref[...] = jnp.dot(
            place, back[...].reshape(ranks * slots, cols), preferred_element_type=jnp.float32
        ).astype(jnp.bfloat16)
        for sem, size in pending.values():
            wait_of(bulk(size), sem).wait_send()


def solution(mesh):
    ep_count, tp_count = mesh.shape["ep"], mesh.shape["tp"]

    def on_device(
        hidden_in, norm_gain, group_ids, inner_ids, group_prob, expert_prob, w_gate, w_up, w_down
    ):
        tokens = hidden_in.shape[0]
        experts, depth, hidden = w_gate.shape
        cols = w_down.shape[2]
        ranks, cap = EPG // experts, tokens // 2
        groups, ys = ep_count // ranks, tp_count // CORES
        feats, side = depth // tp_count, depth // CORES
        others = max(groups - 1, 1)
        hbm = pl.BlockSpec(memory_space=pl.ANY)
        dma = pltpu.SemaphoreType.DMA
        small = (
            hidden_in, norm_gain.reshape(1, depth), group_ids.reshape(1, tokens), inner_ids.T,
            group_prob.reshape(1, tokens), expert_prob.T,
        )
        return pl.pallas_call(
            functools.partial(moe_kernel, ep_count, tp_count),
            out_shape=pltpu.VMEM((tokens, cols), jnp.bfloat16),
            in_specs=[hbm] * 9,
            out_specs=pl.BlockSpec(memory_space=pltpu.VMEM),
            scratch_shapes=[pltpu.VMEM(a.shape, a.dtype) for a in small] + [
                pltpu.VMEM(w_gate.shape, jnp.bfloat16),
                pltpu.VMEM(w_up.shape, jnp.bfloat16),
                pltpu.VMEM(w_down.shape, jnp.bfloat16),
                pltpu.VMEM((others, cap, feats + LANES), jnp.bfloat16),
                pltpu.VMEM((CORES, ranks * cap, side + LANES), jnp.bfloat16),
                pltpu.VMEM((groups, CORES, ys, ranks * cap, feats + LANES), jnp.bfloat16),
                pltpu.VMEM((groups, CORES, ys, ranks * cap, experts * hidden), jnp.bfloat16),
                pltpu.VMEM((groups, ranks * cap, cols), jnp.bfloat16),
                pltpu.VMEM((groups, ranks, cap, cols), jnp.bfloat16),
                dma((len(small),)), dma((3,)), dma((groups,)),
                dma((others,)), dma((ranks - 1,)), dma((1,)),
                dma((others, ranks * ys - 1)), dma((others, ys + 1)),
                dma((ys - 1,)), dma((groups, CHUNKS, ys)),
                dma((others, CHUNKS, CORES, ys - 1)), dma((groups,)),
            ],
            compiler_params=pltpu.CompilerParams(
                collective_id=0, has_side_effects=True, vmem_limit_bytes=56 * 1024 * 1024
            ),
        )(*small, w_gate, w_up, w_down)

    placed = (
        P("ep", None), P(), P("ep"), P("ep", None), P("ep"), P("ep", None),
        P("ep", None, "tp"), P("ep", None, "tp"), P("ep", None, "tp"),
    )
    return jax.shard_map(
        on_device, mesh=mesh, in_specs=placed, out_specs=P("ep", "tp"), check_vma=False
    )
```
